32 devices in a mesh: ep: 16 (over z, y, x), tp: 2 (over core).
Axes of the slice: x: 2, y: 2, z: 4, core: 2. Of those that a mesh axis runs over, the one named last changes fastest.
Arguments:
- tokens: bfloat16 [6144, 3072], P('ep', 'tp'), may hold values from -6 to 6
- cotangent: bfloat16 [6144, 3072], P('ep', 'tp'), may hold values from -6 to 6
- experts: int32 [6144, 2], P('ep'), may hold values from 0 to 15, all different within a row; in each aligned block of 384 rows (0 to 383, 384 to 767, ...) at most 72 rows name the same one
- gate: float32 [6144, 2], P('ep'), may hold values from 0.2 to 1
- w_gate: bfloat16 [16, 3072, 768], P('ep', None, 'tp'), may hold values from -0.109375 to 0.109375
- w_up: bfloat16 [16, 3072, 768], P('ep', None, 'tp'), may hold values from -0.109375 to 0.109375
- w_down: bfloat16 [16, 768, 3072], P('ep', 'tp'), may hold values from -0.21875 to 0.21875
Outputs:
- token_grad: bfloat16 [6144, 3072], P('ep', 'tp')
- gate_grad: float32 [6144, 2], P('ep')
- gate_weight_grad: bfloat16 [16, 3072, 768], P('ep', None, 'tp')
- up_weight_grad: bfloat16 [16, 3072, 768], P('ep', None, 'tp')
- down_weight_grad: bfloat16 [16, 768, 3072], P('ep', 'tp')
- gate_row_norms: float32 [16, 3072], P('ep')
- up_row_norms: float32 [16, 3072], P('ep')
- down_row_norms: float32 [16, 768], P('ep', 'tp')
The draws below stay inside these ranges and needn't reach their ends.
Inputs may be any that keep to these rules, and one draw needn't show every extreme that they name: A row names 2 different experts. In each aligned block of 384 rows (the rows of one index of ep) no expert is named by more than 72 rows, a bound that some block reaches.
All inputs are finite; a program needn't handle non-finite values.
Results may differ from the reference program's by a relative error of at most 0.008.
Values may be sent and summed in bfloat16 or wider, within the bound.
A program may use at most 128 MiB of HBM per device.

```python
import math
import jax
import jax.numpy as jnp
import numpy as np
from jax import lax

D = 3072
F = 768
TOP = 2
TOK_EP = 384
EXPERTS = 16
CAP = 72
TOKENS = 6144
N_EP = 16
N_TP = 2


def shard_levels(own_key, extent, cuts, low, high):
    def one(position, blocks):
        steps = jax.random.uniform(jax.random.fold_in(jax.random.fold_in(own_key, 6), position), (blocks,), jnp.float32, low / len(cuts), high / len(cuts))
        return jnp.repeat(jnp.exp(steps), extent[position] // blocks).reshape((-1,) + (1,) * (len(extent) - position - 1))

    loudness = one(*cuts[0])
    for cut in cuts[1:]:
        loudness = loudness * one(*cut)
    return loudness


def deal_out(own_key, own, number, rows, amount, top, limit, slope):
    order = jax.random.permutation(own_key, amount)
    packed, ordinary = portions_of(amount, rows * top, limit, slope, True), portions_of(amount, rows * top, limit, slope, False)
    places = jnp.arange(amount)

    def named(lengths, offset_by):
        used = int((lengths > 0).sum())
        fixed = max(1, used // 4)
        moved = fixed + (places - fixed + offset_by * (used - fixed)) % max(1, amount - fixed)
        return jnp.zeros((amount,), jnp.int32).at[order[jnp.where(places < fixed, places, moved)]].set(jnp.asarray(lengths, jnp.int32))

    lengths = jnp.where(number % 4 == 0, named(packed, number // 4), named(ordinary, number - number // 4 - 1))
    mixed = jax.random.permutation(jax.random.fold_in(own, 3), amount)
    donor, taker = mixed[0:amount // 2 * 2:2], mixed[1:amount // 2 * 2:2]
    margin = jnp.minimum(lengths[donor] - 1, limit - lengths[taker]) // 2
    margin = jnp.where((donor == order[0]) | (taker == order[0]) | (lengths[taker] == 0), 0, jnp.maximum(margin, 0))
    moved = jax.random.randint(jax.random.fold_in(own, 4), (amount // 2,), 0, 1 << 20) % (margin + 1)
    lengths = lengths.at[donor].add(-moved).at[taker].add(moved)
    members = jnp.searchsorted(jnp.cumsum(lengths), jnp.arange(rows * top), side="right").astype(jnp.int32)
    listing = members.reshape(top, rows).T
    listing = listing[jax.random.permutation(jax.random.fold_in(own, 1), rows)]
    offset_by = jax.random.randint(jax.random.fold_in(own, 2), (rows, 1), 0, top)
    return jnp.take_along_axis(listing, (jnp.arange(top)[None, :] + offset_by) % top, axis=1)


def portions_of(count, total, reach, lean, full):
    portions = [(1 << 20) // math.isqrt(grade ** lean) + 1 for grade in range(1, count + 1)]
    largest = reach if full else min(reach, max(-(-total // count), total * portions[0] // sum(portions)))
    least = 1 if total - largest >= count - 1 else 0
    holding, spare = [largest] + [least] * (count - 1), total - largest - least * (count - 1)
    while spare > 0:
        candidates = [i for i in range(1, count) if holding[i] < largest] or [i for i in range(1, count) if holding[i] < reach]
        mass, budget = sum([portions[i] for i in candidates]), spare
        for i in candidates:
            addition = min(reach - holding[i], max(1, budget * portions[i] // mass), spare)
            holding[i] = holding[i] + addition
            spare = spare - addition
    return np.array(holding)


def centred(stream_key, shape, deviation, most, split=(), held_as=jnp.bfloat16):
    entries = jax.random.normal(stream_key, shape, jnp.float32) * deviation
    if len(split) > 0:
        entries = shard_levels(stream_key, shape, split, -0.22, 0.18) * entries
    return jnp.clip(entries, min=-most, max=most).astype(held_as)


def setup_inputs(seed: int = 0) -> dict:
    seeds = jax.random.split(jax.random.key(seed), 8)
    tokens = centred(seeds[0], (TOKENS, D), 1.0, 6.0, ((0, 16), (1, 2)))
    cotangent = centred(seeds[1], (TOKENS, D), 1.0, 6.0, ((0, 16), (1, 2)))
    experts_keys = jax.random.split(jax.random.fold_in(seeds[2], 1), TOKENS // TOK_EP)
    experts_turns = jax.random.permutation(jax.random.fold_in(seeds[2], 3), TOKENS // TOK_EP)
    experts = jax.vmap(lambda own, number: deal_out(jax.random.fold_in(seeds[2], 2), own, number, TOK_EP, EXPERTS, TOP, CAP, 2))(experts_keys, experts_turns).reshape((TOKENS, TOP))
    gate = jnp.clip(0.2 + 0.8 * jax.random.uniform(seeds[3], (TOKENS, TOP), jnp.float32) ** shard_levels(seeds[3], (TOKENS, TOP), ((0, 16),), -0.2, 0.2), 0.2, 1.0)
    w_gate = centred(seeds[4], (EXPERTS, D, F), D ** -0.5, 0.109375, ((0, 16), (2, 2)))
    w_up = centred(seeds[5], (EXPERTS, D, F), D ** -0.5, 0.109375, ((0, 16), (2, 2)))
    w_down = centred(seeds[6], (EXPERTS, F, D), F ** -0.5, 0.21875, ((0, 16), (1, 2)))
    return dict(tokens=tokens, cotangent=cotangent, experts=experts, gate=gate, w_gate=w_gate, w_up=w_up, w_down=w_down)


def slot_table(route_block, experts_count, cap):
    pair_ids = route_block.reshape(-1).astype(jnp.int32)
    pair_count = pair_ids.shape[0]
    onehot = (pair_ids[:, None] == jnp.arange(experts_count, dtype=jnp.int32)[None, :]).astype(jnp.int32)
    ranking = jnp.sum(jnp.cumsum(onehot, axis=0) * onehot, axis=1) - 1
    slot_of = (pair_ids * cap + ranking).astype(jnp.int32)
    slot_pairs = jnp.full((experts_count * cap,), pair_count, jnp.int32).at[slot_of].set(
        jnp.arange(pair_count, dtype=jnp.int32))
    return slot_of, slot_pairs


def expert_terms(rows_in, rows_cot, gate_mat, up_mat, down_mat):
    contract_last = (((1,), (1,)), ((), ()))
    contract_rows = (((0,), (0,)), ((), ()))
    gate_pre = jnp.dot(rows_in, gate_mat, preferred_element_type=jnp.float32)
    up_pre = jnp.dot(rows_in, up_mat, preferred_element_type=jnp.float32)
    sigma = jax.nn.sigmoid(gate_pre)
    active = gate_pre * sigma
    hidden = (active * up_pre).astype(jnp.bfloat16)
    hidden_grad = lax.dot_general(rows_cot, down_mat, contract_last, preferred_element_type=jnp.float32)
    products = jnp.sum(hidden.astype(jnp.float32) * hidden_grad, axis=1).astype(jnp.bfloat16)
    gate_grad_pre = (hidden_grad * up_pre * sigma * (1.0 + gate_pre * (1.0 - sigma))).astype(jnp.bfloat16)
    up_grad_pre = (hidden_grad * active).astype(jnp.bfloat16)
    block = F // N_TP
    total = jnp.zeros((rows_in.shape[0], D), jnp.float32)
    for index in range(N_TP):
        lower = index * block
        upper = lower + block
        piece = lax.dot_general(gate_grad_pre[:, lower:upper], gate_mat[:, lower:upper], contract_last,
                                preferred_element_type=jnp.float32)
        piece = piece + lax.dot_general(up_grad_pre[:, lower:upper], up_mat[:, lower:upper], contract_last,
                                        preferred_element_type=jnp.float32)
        rounded = lax.optimization_barrier(piece.astype(jnp.bfloat16))
        total = total + rounded.astype(jnp.float32)
    route_rows = total.astype(jnp.bfloat16)
    gate_sum = lax.dot_general(rows_in, gate_grad_pre, contract_rows, preferred_element_type=jnp.float32)
    up_sum = lax.dot_general(rows_in, up_grad_pre, contract_rows, preferred_element_type=jnp.float32)
    down_sum = lax.dot_general(hidden, rows_cot, contract_rows, preferred_element_type=jnp.float32)
    return (route_rows, products, gate_sum.astype(jnp.bfloat16), up_sum.astype(jnp.bfloat16),
            down_sum.astype(jnp.bfloat16), jnp.sum(gate_sum * gate_sum, axis=1),
            jnp.sum(up_sum * up_sum, axis=1), jnp.sum(down_sum * down_sum, axis=1))


def reference(tokens, cotangent, experts, gate, w_gate, w_up, w_down):
    pair_total = TOKENS * TOP
    pair_block = TOK_EP * TOP
    routes = experts.reshape(N_EP, TOK_EP, TOP)
    slot_of, slot_pairs = jax.vmap(lambda block_routes: slot_table(block_routes, EXPERTS, CAP))(routes)
    offsets = (jnp.arange(N_EP, dtype=jnp.int32) * pair_block)[:, None]
    global_pairs = jnp.where(slot_pairs < pair_block, slot_pairs + offsets, pair_total).astype(jnp.int32)
    by_expert = global_pairs.reshape(N_EP, EXPERTS, CAP).transpose(1, 0, 2).reshape(EXPERTS, N_EP * CAP)
    weighted = (gate[:, :, None] * cotangent.astype(jnp.float32)[:, None, :]).astype(jnp.bfloat16)
    padding = jnp.zeros((1, D), jnp.bfloat16)
    token_pad = jnp.concatenate([tokens, padding], axis=0)
    weighted_pad = jnp.concatenate([weighted.reshape(pair_total, D), padding], axis=0)

    def per_expert(operands):
        indices, gate_mat, up_mat, down_mat = operands
        rows_in = token_pad[indices // TOP]
        rows_cot = weighted_pad[indices]
        return expert_terms(rows_in, rows_cot, gate_mat, up_mat, down_mat)

    results = lax.map(per_expert, (by_expert, w_gate, w_up, w_down))
    route_rows, products = results[0], results[1]
    flat_index = by_expert.reshape(-1)
    pair_rows = jnp.zeros((pair_total + 1, D), jnp.bfloat16).at[flat_index].set(route_rows.reshape(-1, D))
    pair_products = jnp.zeros((pair_total + 1,), jnp.bfloat16).at[flat_index].set(products.reshape(-1))
    token_grad = jnp.sum(pair_rows[:pair_total].astype(jnp.float32).reshape(TOKENS, TOP, D), axis=1)
    gate_grad = pair_products[:pair_total].astype(jnp.float32).reshape(TOKENS, TOP) / gate
    return (token_grad.astype(jnp.bfloat16), gate_grad, results[2], results[3], results[4],
            results[5], results[6], results[7])
```

```python
import jax
import jax.numpy as jnp
from jax import lax
from jax.sharding import PartitionSpec as P

F32 = jnp.float32
BF16 = jnp.bfloat16
LAST = (((1,), (1,)), ((), ()))
ROWS = (((0,), (0,)), ((), ()))


def slots_of(routes, groups, cap):
    rows = routes.shape[1]
    ids = lax.broadcasted_iota(jnp.int32, (groups, rows), 0)
    hits = [routes[k][None, :] == ids for k in range(routes.shape[0])]
    named = sum(h.astype(F32) for h in hits).astype(BF16)
    before = (
        lax.broadcasted_iota(jnp.int32, (rows, rows), 0)
        < lax.broadcasted_iota(jnp.int32, (rows, rows), 1)
    ).astype(BF16)
    rank = jnp.dot(named, before, preferred_element_type=F32)
    return jnp.stack(
        [routes[k] * cap + jnp.sum(jnp.where(h, rank, 0.0), axis=0).astype(jnp.int32) for k, h in enumerate(hits)]
    )


def per_device(tokens, cotangent, experts, gate, w_gate, w_up, w_down):
    groups = lax.axis_size("ep")
    tok_rows, top = experts.shape
    cap = 3 * tok_rows * top // (2 * groups)
    total = groups * cap
    half = tokens.shape[1]
    core = lax.axis_index("tp")
    swap = [(0, 1), (1, 0)]
    slot = slots_of(experts.T, groups, cap)
    gate_t = gate.T
    slot_ids = lax.broadcasted_iota(jnp.int32, (total, tok_rows), 0)
    match = [slot[k][None, :] == slot_ids for k in range(top)]
    pick = sum(m.astype(F32) for m in match).astype(BF16)
    slot_gate = sum(
        jnp.sum(jnp.where(m, gate_t[k][None, :], 0.0), axis=1, keepdims=True) for k, m in enumerate(match)
    )
    pick, slot_gate = lax.optimization_barrier((pick, slot_gate))

    def exchange(x):
        y = lax.all_to_all(x.reshape(groups, cap, -1), "ep", split_axis=0, concat_axis=0, tiled=True)
        return y.reshape(total, -1)

    sent_tok = jnp.dot(pick, tokens, preferred_element_type=F32).astype(BF16)
    own_tok = exchange(sent_tok)
    cot = jnp.dot(pick, cotangent, preferred_element_type=F32)
    sent_cot = (cot * slot_gate).astype(BF16)
    own_cot = exchange(sent_cot)

    def both(own, other):
        return jnp.where(
            core == 0,
            jnp.concatenate([own, other], axis=1),
            jnp.concatenate([other, own], axis=1),
        )

    w_in = jnp.concatenate([w_gate[0], w_up[0]], axis=1)
    hid = w_gate.shape[2]
    w_mine = lax.dynamic_slice_in_dim(w_in, core * half, half, 0)
    w_other = lax.dynamic_slice_in_dim(w_in, (1 - core) * half, half, 0)
    d_mine = lax.dynamic_slice_in_dim(w_down[0], core * half, half, 1)
    d_other = lax.dynamic_slice_in_dim(w_down[0], (1 - core) * half, half, 1)

    other_tok = lax.ppermute(own_tok, "tp", swap)
    rows_in = both(own_tok, other_tok)
    pre = jnp.dot(rows_in, w_in, preferred_element_type=F32)
    other_cot = lax.ppermute(own_cot, "tp", swap)
    grad_mine = lax.dot_general(own_cot, d_mine, LAST, preferred_element_type=F32)
    hidden_grad = grad_mine + lax.dot_general(other_cot, d_other, LAST, preferred_element_type=F32)
    gate_pre, up_pre = pre[:, :hid], pre[:, hid:]
    sigma = jax.nn.sigmoid(gate_pre)
    active = gate_pre * sigma
    hidden = (active * up_pre).astype(BF16)
    product_part = jnp.sum(hidden.astype(F32) * hidden_grad, axis=1)
    grads = jnp.concatenate(
        [
            (hidden_grad * up_pre * sigma * (1.0 + gate_pre * (1.0 - sigma))).astype(BF16),
            (hidden_grad * active).astype(BF16),
        ],
        axis=1,
    )
    part_other = lax.dot_general(grads, w_other, LAST, preferred_element_type=F32).astype(BF16)
    arrived = lax.ppermute(part_other, "tp", swap)
    part_mine = lax.dot_general(grads, w_mine, LAST, preferred_element_type=F32)
    row_grads = (part_mine + arrived.astype(F32)).astype(BF16)
    high = product_part.astype(BF16)
    low = (product_part - high.astype(F32)).astype(BF16)
    lane = lax.broadcasted_iota(jnp.int32, (total, 128), 1)
    spare = jnp.where(lane == 0, high[:, None], jnp.where(lane == 1, low[:, None], jnp.zeros((), BF16)))
    row_grads = jnp.concatenate([row_grads, spare], axis=1)
    back = exchange(row_grads)

    rows_in, grads, other_cot, hidden, row_grads = lax.optimization_barrier(
        (rows_in, grads, other_cot, hidden, row_grads)
    )
    gate_sum = lax.dot_general(rows_in, grads[:, :hid], ROWS, preferred_element_type=F32)
    up_sum = lax.dot_general(rows_in, grads[:, hid:], ROWS, preferred_element_type=F32)
    rows_cot = both(own_cot, other_cot)
    down_sum = lax.dot_general(hidden, rows_cot, ROWS, preferred_element_type=F32)
    in_norms = jnp.stack([jnp.sum(gate_sum * gate_sum, axis=1), jnp.sum(up_sum * up_sum, axis=1)])
    down_norms = jnp.sum(down_sum * down_sum, axis=1)
    in_norms = in_norms + lax.ppermute(in_norms, "tp", swap)
    pair = lax.dot_general(
        back[:, half:], jnp.concatenate([match[k] for k in range(top)], axis=1).astype(BF16), ROWS,
        preferred_element_type=F32,
    )
    route_products = (pair[0] + pair[1]).reshape(top, tok_rows)
    route_products = route_products + lax.ppermute(route_products, "tp", swap)
    gate_grad = (route_products.astype(BF16).astype(F32) / gate_t).T
    token_grad = lax.dot_general(pick, back[:, :half], ROWS, preferred_element_type=F32).astype(BF16)
    return (
        token_grad,
        gate_grad,
        gate_sum.astype(BF16)[None],
        up_sum.astype(BF16)[None],
        down_sum.astype(BF16)[None],
        in_norms[0][None],
        in_norms[1][None],
        down_norms[None],
    )


def solution(mesh):
    placed = (
        P("ep", "tp"),
        P("ep", "tp"),
        P("ep", None),
        P("ep", None),
        P("ep", None, "tp"),
        P("ep", None, "tp"),
        P("ep", "tp", None),
    )
    return jax.shard_map(
        per_device,
        mesh=mesh,
        in_specs=placed,
        out_specs=(
            P("ep", "tp"),
            P("ep", None),
            P("ep", None, "tp"),
            P("ep", None, "tp"),
            P("ep", "tp", None),
            P("ep", None),
            P("ep", None),
            P("ep", "tp"),
        ),
        check_vma=False,
    )
```
